768 devices in a mesh: sp: 384 (over z, y, x), tp: 2 (over core).
Axes of the slice: x: 4, y: 8, z: 12, core: 2. Of those that a mesh axis runs over, the one named last changes fastest.
Arguments:
- tokens: bfloat16 [98304, 2048], P('sp'), may hold values from -6 to 6
- query_weight: bfloat16 [2, 2048, 512], P(None, None, 'tp'), may hold values from -0.125 to 0.125
- key_weight: bfloat16 [2, 2048, 512], P(None, None, 'tp'), may hold values from -0.125 to 0.125
- value_weight: bfloat16 [2, 2048, 512], P(None, None, 'tp'), may hold values from -0.125 to 0.125
- out_weight: bfloat16 [2, 512, 2048], replicated, may hold values from -1.5 to 1.5
- rel_table: float32 [2, 8, 257], P(None, 'tp'), may hold values from -5 to 262
- norm_gain: float32 [2, 2048], replicated, may hold values from 0.1 to 1.9
- norm_bias: float32 [2, 2048], replicated, may hold values from -1.5 to 1.5
Outputs:
- encoded: bfloat16 [98304, 2048], P('sp', 'tp')
The draws below stay inside these ranges and needn't reach their ends.
All inputs are finite; a program needn't handle non-finite values.
Results may differ from the reference program's by a relative error of at most 0.0095.
Values may be sent and summed in bfloat16 or wider, within the bound.
No kernel may reach another device: no remote copies, remote signals or barrier semaphores. Data moves between devices by JAX's collectives and lax.ppermute only.
A program may use at most 64 MiB of HBM per device.

```python
import jax
import jax.numpy as jnp
from jax import lax

D = 2048
HEADS = 8
HEAD_DIM = 64
SEG = 64
LEFT = 4
CLIP = 128
LAYERS = 2
HW = 512
TOKENS = 98304


def draw_rel_table(key, part):
    shape = (LAYERS, HEADS, 2 * CLIP + 1)
    return jnp.clip(jax.random.normal(key, shape, jnp.float32), -5.0, 5.0)


def block_scale(key, dims, split, low, largest):
    level, own = 1.0, jax.random.fold_in(key, 6)
    for position, parts in split:
        draws = jnp.exp(jax.random.uniform(jax.random.fold_in(own, position), (parts,), jnp.float32, low / len(split), largest / len(split)))
        level = level * jnp.repeat(draws, dims[position] // parts).reshape([-1 if axis == position else 1 for axis in range(len(dims))])
    return level


def gaussian(key, shape, scale, most, cuts=(), held_as=jnp.bfloat16):
    level = block_scale(key, shape, cuts, -0.22, 0.18) if cuts else 1.0
    values = jax.random.normal(key, shape, jnp.float32) * scale * level
    return jnp.minimum(jnp.maximum(values, -most), most).astype(held_as)


def setup_inputs(seed: int = 0) -> dict:
    seeds = jax.random.split(jax.random.key(seed), 9)
    return {
        "tokens": gaussian(seeds[0], (TOKENS, D), 1.0, 6.0, ((0, 384),)),
        "query_weight": gaussian(seeds[1], (LAYERS, D, HW), D ** -0.5, 0.125, ((2, 2),)),
        "key_weight": gaussian(seeds[2], (LAYERS, D, HW), D ** -0.5, 0.125, ((2, 2),)),
        "value_weight": gaussian(seeds[3], (LAYERS, D, HW), D ** -0.5, 0.125, ((2, 2),)),
        "out_weight": gaussian(seeds[4], (LAYERS, HW, D), (HW // 32) ** -0.5, 1.5),
        "rel_table": draw_rel_table(jax.random.fold_in(seeds[8], 71), 0),
        "norm_gain": jnp.clip(1.0 + 0.18 * jax.random.normal(seeds[6], (LAYERS, D), jnp.float32), 0.1, 1.9),
        "norm_bias": gaussian(seeds[7], (LAYERS, D), 0.3, 1.5, (), jnp.float32),
    }


residual_scale = 2.0 ** 0.5
norm_eps = 1e-05
masked_score = -1e+30

def post_norm(previous, mixed, gain, shift):
    total = residual_scale * previous.astype(jnp.float32) + mixed
    mean = lax.optimization_barrier(jnp.mean(total, -1, keepdims=True))
    centred = total - mean
    variance = lax.optimization_barrier(jnp.mean(centred * centred, -1, keepdims=True))
    return (centred * lax.rsqrt(variance + norm_eps) * gain + shift).astype(jnp.bfloat16)

def band_attention(query, keys, values, table):
    reach = LEFT * SEG
    band = reach + SEG
    seg_count = TOKENS // SEG
    query3 = query.reshape(TOKENS, HEADS, HEAD_DIM)
    zeros = jnp.zeros((reach, HEADS, HEAD_DIM), jnp.bfloat16)
    padded_keys = jnp.concatenate([zeros, keys.reshape(TOKENS, HEADS, HEAD_DIM)], axis=0)
    padded_values = jnp.concatenate([zeros, values.reshape(TOKENS, HEADS, HEAD_DIM)], axis=0)
    distance = reach + jnp.arange(SEG, dtype=jnp.int32)[:, None] - jnp.arange(band, dtype=jnp.int32)[None, :]
    column = jnp.clip(distance, -CLIP, CLIP) + CLIP
    bias = table.astype(jnp.float32)[:, column]

    def one_segment(index):
        start = (index * SEG).astype(jnp.int32)
        query_block = lax.dynamic_slice_in_dim(query3, start, SEG, 0).astype(jnp.float32)
        key_band = lax.dynamic_slice_in_dim(padded_keys, start, band, 0).astype(jnp.float32)
        value_band = lax.dynamic_slice_in_dim(padded_values, start, band, 0).astype(jnp.float32)
        scores = jnp.einsum('qhd,khd->hqk', query_block, key_band) * HEAD_DIM ** (-0.5) + bias
        key_position = start - reach + jnp.arange(band, dtype=jnp.int32)
        scores = jnp.where((key_position >= 0)[None, None, :], scores, masked_score)
        peak = lax.optimization_barrier(jnp.max(scores, -1, keepdims=True))
        expo = jnp.exp(scores - peak)
        weights = (expo / lax.optimization_barrier(jnp.sum(expo, -1, keepdims=True))).astype(jnp.bfloat16)
        attended = jnp.einsum('hqk,khd->qhd', weights.astype(jnp.float32), value_band)
        return attended.astype(jnp.bfloat16)
    blocks = lax.map(one_segment, jnp.arange(seg_count, dtype=jnp.int32))
    return blocks.reshape(TOKENS, HEADS * HEAD_DIM)

def reference(tokens, query_weight, key_weight, value_weight, out_weight, rel_table, norm_gain, norm_bias):
    hidden = tokens
    for layer_index in range(LAYERS):
        query = jnp.dot(hidden, query_weight[layer_index], preferred_element_type=jnp.float32).astype(jnp.bfloat16)
        keys = jnp.dot(hidden, key_weight[layer_index], preferred_element_type=jnp.float32).astype(jnp.bfloat16)
        values = jnp.dot(hidden, value_weight[layer_index], preferred_element_type=jnp.float32).astype(jnp.bfloat16)
        attended = band_attention(query, keys, values, rel_table[layer_index])
        mixed = jnp.dot(attended, out_weight[layer_index], preferred_element_type=jnp.float32)
        hidden = post_norm(hidden, mixed, norm_gain[layer_index], norm_bias[layer_index])
    return hidden
```

```python
import functools

import jax
import jax.numpy as jnp
from jax import lax
from jax.experimental import pallas as pl
from jax.experimental.pallas import tpu as pltpu
from jax.sharding import PartitionSpec as P

SEG = 64
LEFT = 4
CLIP = 128
LAYERS = 2
REACH = LEFT * SEG
BAND = REACH + SEG
SPAN = 384

residual_scale = 2.0**0.5
norm_eps = 1e-05
masked_score = -1e30

VM = pl.BlockSpec(memory_space=pltpu.VMEM)
SM = pl.BlockSpec(memory_space=pltpu.SMEM)
ANY = pl.BlockSpec(memory_space=pltpu.HBM)
bf16 = jnp.bfloat16
f32 = jnp.float32


def kernel_call(body, name, outs, specs, args, scratch=(), limit=24 << 20, flops=10**9):
    return pl.pallas_call(
        body,
        name=name,
        out_shape=[jax.ShapeDtypeStruct(s, d) for s, d in outs],
        in_specs=specs,
        out_specs=[VM] * len(outs),
        scratch_shapes=scratch,
        compiler_params=pltpu.CompilerParams(vmem_limit_bytes=limit),
        cost_estimate=pl.CostEstimate(flops=flops, transcendentals=0, bytes_accessed=1 << 20),
    )(*args)


def matmul(a, b):
    return jnp.dot(a, b, preferred_element_type=f32)


def first_kv(tok, wk, wv, kv, tokv, wks, wvs, sem):
    rows, width = tok.shape
    heads = wk.shape[2]
    parts = sem.shape[1]
    step = width // parts
    copies = []
    for c in range(parts):
        cut = pl.ds(c * step, step)
        trio = (
            pltpu.make_async_copy(tok.at[:, cut], tokv.at[:, cut], sem.at[0, c]),
            pltpu.make_async_copy(wk.at[0, cut, :], wks.at[cut, :], sem.at[1, c]),
            pltpu.make_async_copy(wv.at[0, cut, :], wvs.at[cut, :], sem.at[2, c]),
        )
        for copy in trio:
            copy.start()
        copies.append(trio)
    keys = values = None
    for c in range(parts):
        for copy in copies[c]:
            copy.wait()
        cut = pl.ds(c * step, step)
        x = tokv[:, cut]
        k = matmul(x, wks[cut, :])
        v = matmul(x, wvs[cut, :])
        keys = k if keys is None else keys + k
        values = v if values is None else values + v
    kv[:, :heads] = keys.astype(bf16)
    kv[:, heads:] = values.astype(bf16)


def fill_bias(table, bias):
    rows, cols = table.shape
    t = table[...]
    head = t[:, : cols - 1]
    offset = lax.broadcasted_iota(jnp.int32, (cols - 1, SPAN), 1)
    index = lax.broadcasted_iota(jnp.int32, (cols - 1, SPAN), 0)
    onehot = (jnp.clip(REACH + SEG - 1 - offset, -CLIP, CLIP) + CLIP == index).astype(f32).astype(bf16)
    high = head.astype(bf16)
    rest = head - high.astype(f32)
    mid = rest.astype(bf16)
    low = (rest - mid.astype(f32)).astype(bf16)
    by_offset = matmul(high, onehot) + matmul(mid, onehot) + matmul(low, onehot)
    far = lax.broadcasted_iota(jnp.int32, (rows, SPAN), 1) <= REACH + SEG - 1 - CLIP
    by_offset = jnp.where(far, t[:, cols - 1 :], by_offset)
    for r in range(rows):
        line = jnp.broadcast_to(by_offset[r : r + 1, :], (SEG, SPAN))
        skew = pltpu.roll(line, SPAN - (SEG - 1), 1, stride=1, stride_axis=0)
        bias[r * SEG : (r + 1) * SEG, :] = skew


def first_query(tokv, wq, wo, wk, wv, table, q, bias, wo0, wq1, wk1, wv1, wo1, wqs, sem):
    width = tokv.shape[1]
    copies = [
        pltpu.make_async_copy(wq.at[0], wqs, sem.at[0]),
        pltpu.make_async_copy(wo.at[0], wo0, sem.at[1]),
        pltpu.make_async_copy(wk.at[1], wk1, sem.at[2]),
        pltpu.make_async_copy(wv.at[1], wv1, sem.at[3]),
        pltpu.make_async_copy(wq.at[1], wq1, sem.at[4]),
        pltpu.make_async_copy(wo.at[1], wo1, sem.at[5]),
    ]
    for copy in copies:
        copy.start()
    fill_bias(table, bias)
    copies[0].wait()
    q[...] = (matmul(tokv[...], wqs[...]).astype(bf16).astype(f32) * 0.125).astype(bf16)
    for copy in copies[1:]:
        copy.wait()


def later_query(x, wq, q):
    q[...] = (matmul(x[...], wq[...]).astype(bf16).astype(f32) * 0.125).astype(bf16)


def attention(layer, place, q, own, prev, bias, out, ext):
    rows, width = q.shape
    heads = width // 64
    ext[:rows, :] = prev[...]
    ext[rows:, :] = own[...]
    lane = lax.broadcasted_iota(jnp.int32, (SEG, width), 1) // 64
    column = lax.broadcasted_iota(jnp.int32, (1, BAND), 1)
    blocked = jnp.where(place[0] == 0, masked_score, 0.0)
    for i in range(rows // SEG):
        qs = q[i * SEG : (i + 1) * SEG, :]
        stack = jnp.concatenate(
            [jnp.where(lane == h, qs, jnp.zeros_like(qs)) for h in range(heads)], axis=0
        )
        keys = ext[i * SEG : i * SEG + BAND, :width]
        values = ext[i * SEG : i * SEG + BAND, width:]
        score = lax.dot_general(stack, keys, (((1,), (1,)), ((), ())), preferred_element_type=f32)
        score = score + bias[layer * heads * SEG : (layer + 1) * heads * SEG, :BAND]
        score = score + jnp.where(column < REACH - i * SEG, blocked, 0.0)
        peak = jnp.max(score, -1, keepdims=True)
        expo = jnp.exp(score - peak)
        scale = 1.0 / jnp.sum(expo, -1, keepdims=True)
        mixed = matmul(expo.astype(bf16), values) * scale
        total = None
        for h in range(heads):
            part = jnp.where(lane == h, mixed[h * SEG : (h + 1) * SEG, :], 0.0)
            total = part if total is None else total + part
        out[i * SEG : (i + 1) * SEG, :] = total.astype(bf16)


def out_project(att, wo, x, total):
    width = x.shape[1]
    step = 512
    a = att[...]
    acc = None
    for c in range(width // step):
        cut = slice(c * step, (c + 1) * step)
        t = residual_scale * x[:, cut].astype(f32) + matmul(a, wo[:, cut])
        total[:, cut] = t
        s = jnp.sum(t, -1, keepdims=True)
        acc = s if acc is None else acc + s
    mean = acc * (1.0 / width)
    acc = None
    for c in range(width // step):
        cut = slice(c * step, (c + 1) * step)
        d = total[:, cut] - mean
        s = jnp.sum(d * d, -1, keepdims=True)
        acc = s if acc is None else acc + s
    return mean, lax.rsqrt(acc * (1.0 / width) + norm_eps)


def middle(layer, att, wo, x, gain, shift, wk, wv, y, kv, total):
    width = x.shape[1]
    heads = wk.shape[1]
    mean, scale = out_project(att, wo, x, total)
    step = 512
    keys = values = None
    for c in range(width // step):
        cut = slice(c * step, (c + 1) * step)
        d = (total[:, cut] - mean) * scale * gain[layer : layer + 1, cut] + shift[layer : layer + 1, cut]
        d = d.astype(bf16)
        y[:, cut] = d
        k = matmul(d, wk[cut, :])
        v = matmul(d, wv[cut, :])
        keys = k if keys is None else keys + k
        values = v if values is None else values + v
    kv[:, :heads] = keys.astype(bf16)
    kv[:, heads:] = values.astype(bf16)


def last(layer, place, att, wo, x, gain, shift, out, total):
    half = out.shape[1]
    mean, scale = out_project(att, wo, x, total)
    start = pl.multiple_of(place[1] * half, 128)
    cut = pl.ds(start, half)
    g = gain[layer : layer + 1, cut]
    s = shift[layer : layer + 1, cut]
    out[...] = ((total[:, cut] - mean) * scale * g + s).astype(bf16)


def body(tokens, wq, wk, wv, wo, table, gain, shift):
    rows, width = tokens.shape
    cols = wq.shape[2]
    heads = table.shape[1]
    sp = lax.axis_index("sp")
    tp = lax.axis_index("tp")
    place = jnp.stack([sp, tp]).astype(jnp.int32)
    count = lax.axis_size("sp")
    along = [(s, s + 1) for s in range(count - 1)]
    tokens, wq, wk, wv, wo = (
        pltpu.with_memory_space_constraint(a, pltpu.HBM) for a in (tokens, wq, wk, wv, wo)
    )
    flat_table = table.reshape(LAYERS * heads, table.shape[2])

    kv, x = kernel_call(
        first_kv, "kv0", [((rows, 2 * cols), bf16), ((rows, width), bf16)], [ANY, ANY, ANY], (tokens, wk, wv),
        [pltpu.VMEM((width, cols), bf16), pltpu.VMEM((width, cols), bf16), pltpu.SemaphoreType.DMA((3, 4))],
        flops=10**8,
    )
    prev = lax.ppermute(kv, "sp", along)
    q, bias, wo0, wq1, wk1, wv1, wo1 = kernel_call(
        first_query, "q0",
        [((rows, cols), bf16), ((LAYERS * heads * SEG, SPAN), f32), (wo.shape[1:], bf16), (wq.shape[1:], bf16),
         (wq.shape[1:], bf16), (wq.shape[1:], bf16), (wo.shape[1:], bf16)],
        [VM, ANY, ANY, ANY, ANY, VM], (x, wq, wo, wk, wv, flat_table),
        [pltpu.VMEM((width, cols), bf16), pltpu.SemaphoreType.DMA((6,))],
    )
    wouts = (wo0, wo1)
    for layer in range(LAYERS):
        att = kernel_call(
            functools.partial(attention, layer), f"att{layer}", [((rows, cols), bf16)],
            [SM, VM, VM, VM, VM], (place, q, kv, prev, bias),
            [pltpu.VMEM((2 * rows, 2 * cols), bf16)],
        )[0]
        full = lax.all_gather(att, "tp", axis=1, tiled=True)
        if layer + 1 < LAYERS:
            x, kv = kernel_call(
                functools.partial(middle, layer), "mid", [((rows, width), bf16), ((rows, 2 * cols), bf16)],
                [VM] * 7, (full, wouts[layer], x, gain, shift, wk1, wv1),
                [pltpu.VMEM((rows, width), f32)], flops=10**8,
            )
            prev = lax.ppermute(kv, "sp", along)
            q = kernel_call(later_query, "q1", [((rows, cols), bf16)], [VM, VM], (x, wq1))[0]
    return kernel_call(
        functools.partial(last, LAYERS - 1), "end", [((rows, width // 2), bf16)],
        [SM] + [VM] * 5, (place, full, wouts[-1], x, gain, shift),
        [pltpu.VMEM((rows, width), f32)],
    )[0]


def solution(mesh):
    return jax.shard_map(
        body,
        mesh=mesh,
        in_specs=(
            P("sp", None),
            P(None, None, "tp"),
            P(None, None, "tp"),
            P(None, None, "tp"),
            P(),
            P(None, "tp", None),
            P(),
            P(),
        ),
        out_specs=P("sp", "tp"),
        check_vma=False,
    )
```

```python
import functools

import jax
import jax.numpy as jnp
from jax import lax
from jax.experimental import pallas as pl
from jax.experimental.pallas import tpu as pltpu
from jax.sharding import PartitionSpec as P

SEG = 64
LEFT = 4
CLIP = 128
LAYERS = 2
REACH = LEFT * SEG
BAND = REACH + SEG
SPAN = 384

residual_scale = 2.0**0.5
norm_eps = 1e-05
masked_score = -1e30

VM = pl.BlockSpec(memory_space=pltpu.VMEM)
ANY = pl.BlockSpec(memory_space=pltpu.HBM)
bf16 = jnp.bfloat16
f32 = jnp.float32


def kernel_call(body, outs, specs, args, scratch=(), limit=10 << 20, flops=10**9, out_specs=None):
    return pl.pallas_call(
        body,
        out_shape=[jax.ShapeDtypeStruct(s, d) for s, d in outs],
        in_specs=specs,
        out_specs=out_specs or [VM] * len(outs),
        scratch_shapes=scratch,
        compiler_params=pltpu.CompilerParams(vmem_limit_bytes=limit),
        cost_estimate=pl.CostEstimate(flops=flops, transcendentals=0, bytes_accessed=1 << 20),
    )(*args)


def is_late(position):
    even = jnp.logical_and(lax.rem(position, 2) == 0, position > 0)
    return jnp.logical_or(even, position == 1)


def late_position(position):
    return position == 1 or (position % 2 == 0 and position > 0)


def matmul(a, b):
    return jnp.dot(a, b, preferred_element_type=f32)


def when_class(late, run):
    flag = is_late(lax.axis_index("sp"))
    pl.when(flag if late else jnp.logical_not(flag))(run)


def fetch(pairs, sem):
    copies = [pltpu.make_async_copy(a, b, sem.at[i]) for i, (a, b) in enumerate(pairs)]
    for copy in copies:
        copy.start()
    return copies


def first_kv(late, tok, wk, wv, kv, tokv, wks, wvs, sem):
    def run():
        _, width = tok.shape
        heads = wk.shape[2]
        parts = sem.shape[1]
        step = width // parts
        copies = []
        for c in range(parts):
            cut = pl.ds(c * step, step)
            trio = (
                pltpu.make_async_copy(tok.at[:, cut], tokv.at[:, cut], sem.at[0, c]),
                pltpu.make_async_copy(wk.at[0, cut, :], wks.at[cut, :], sem.at[1, c]),
                pltpu.make_async_copy(wv.at[0, cut, :], wvs.at[cut, :], sem.at[2, c]),
            )
            for copy in trio:
                copy.start()
            copies.append(trio)
        keys = values = None
        for c in range(parts):
            for copy in copies[c]:
                copy.wait()
            cut = pl.ds(c * step, step)
            x = tokv[:, cut]
            k = matmul(x, wks[cut, :])
            v = matmul(x, wvs[cut, :])
            keys = k if keys is None else keys + k
            values = v if values is None else values + v
        kv[:, :heads] = keys.astype(bf16)
        kv[:, heads:] = values.astype(bf16)

    when_class(late, run)


def fill_bias(table, bias):
    rows, cols = table.shape
    t = table[...]
    head = t[:, : cols - 1]
    offset = lax.broadcasted_iota(jnp.int32, (cols - 1, SPAN), 1)
    index = lax.broadcasted_iota(jnp.int32, (cols - 1, SPAN), 0)
    onehot = (jnp.clip(REACH + SEG - 1 - offset, -CLIP, CLIP) + CLIP == index).astype(f32).astype(bf16)
    high = head.astype(bf16)
    rest = head - high.astype(f32)
    mid = rest.astype(bf16)
    low = (rest - mid.astype(f32)).astype(bf16)
    by_offset = matmul(high, onehot) + matmul(mid, onehot) + matmul(low, onehot)
    far = lax.broadcasted_iota(jnp.int32, (rows, SPAN), 1) <= REACH + SEG - 1 - CLIP
    by_offset = jnp.where(far, t[:, cols - 1 :], by_offset)
    for r in range(rows):
        line = jnp.broadcast_to(by_offset[r : r + 1, :], (SEG, SPAN))
        skew = pltpu.roll(line, SPAN - (SEG - 1), 1, stride=1, stride_axis=0)
        bias[r * SEG : (r + 1) * SEG, :] = skew


def scaled_query(x, w):
    return (matmul(x, w).astype(bf16).astype(f32) * 0.125).astype(bf16)


def choose(main, late, out):
    def from_main():
        out[...] = main[...]

    def from_late():
        out[...] = late[...]

    when_class(False, from_main)
    when_class(True, from_late)


def first_query(layer, x_main, x_late, wq, wo, wk, wv, table, q, bias, x, wo0, wk1, wv1, wqs, sem):
    copies = fetch(
        ((wq.at[layer], wqs), (wo.at[layer], wo0), (wk.at[layer + 1], wk1), (wv.at[layer + 1], wv1)), sem
    )
    choose(x_main, x_late, x)
    fill_bias(table, bias)
    copies[0].wait()
    q[...] = scaled_query(x[...], wqs[...])
    for copy in copies[1:]:
        copy.wait()


def later_query(layer, x_main, x_late, wq, wo, q, x, wo1, wqs, sem):
    copies = fetch(((wq.at[layer], wqs), (wo.at[layer], wo1)), sem)
    choose(x_main, x_late, x)
    copies[0].wait()
    q[...] = scaled_query(x[...], wqs[...])
    copies[1].wait()


def attend(layer, q, bias, ext, out):
    rows, width = q.shape
    heads = width // 64
    lane = lax.broadcasted_iota(jnp.int32, (SEG, width), 1) // 64
    column = lax.broadcasted_iota(jnp.int32, (1, BAND), 1)
    blocked = jnp.where(lax.axis_index("sp") == 0, masked_score, 0.0)
    for i in range(rows // SEG):
        qs = q[i * SEG : (i + 1) * SEG, :]
        stack = jnp.concatenate(
            [jnp.where(lane == h, qs, jnp.zeros_like(qs)) for h in range(heads)], axis=0
        )
        keys = ext[i * SEG : i * SEG + BAND, :width]
        values = ext[i * SEG : i * SEG + BAND, width:]
        score = lax.dot_general(stack, keys, (((1,), (1,)), ((), ())), preferred_element_type=f32)
        score = score + bias[layer * heads * SEG : (layer + 1) * heads * SEG, :BAND]
        score = score + jnp.where(column < REACH - i * SEG, blocked, 0.0)
        peak = jnp.max(score, -1, keepdims=True)
        expo = jnp.exp(score - peak)
        scale = 1.0 / jnp.sum(expo, -1, keepdims=True)
        mixed = matmul(expo.astype(bf16), values) * scale
        total = None
        for h in range(heads):
            part = jnp.where(lane == h, mixed[h * SEG : (h + 1) * SEG, :], 0.0)
            total = part if total is None else total + part
        out[i * SEG : (i + 1) * SEG, :] = total.astype(bf16)


def choose_source(main, late, out):
    late_source = is_late(lax.axis_index("sp") - 1)

    @pl.when(late_source)
    def _():
        out[...] = late[...]

    @pl.when(jnp.logical_not(late_source))
    def _():
        out[...] = main[...]


def main_attention(layer, q, own, prev, bias, out, ext):
    def run():
        rows = q.shape[0]
        ext[:rows, :] = prev[...]
        ext[rows:, :] = own[...]
        attend(layer, q, bias, ext, out)

    when_class(False, run)


def late_attention(layer, q, own, prev_main, prev_late, bias, out, ext):
    def run():
        rows = q.shape[0]
        choose_source(prev_main, prev_late, ext.at[:rows, :])
        ext[rows:, :] = own[...]
        attend(layer, q, bias, ext, out)

    when_class(True, run)


def final_attention(layer, q, own_main, own_late, prev_main, prev_late, bias, out, ext):
    rows = q.shape[0]
    choose(own_main, own_late, ext.at[rows:, :])
    choose_source(prev_main, prev_late, ext.at[:rows, :])
    attend(layer, q, bias, ext, out)


def out_project(att, wo, x, total):
    width = x.shape[1]
    step = 512
    count = width // step
    a = att[...]
    means, squares = [], []
    for c in range(count):
        cut = slice(c * step, (c + 1) * step)
        t = residual_scale * x[:, cut].astype(f32) + matmul(a, wo[:, cut])
        total[:, cut] = t
        m = jnp.sum(t, -1, keepdims=True) * (1.0 / step)
        d = t - m
        means.append(m)
        squares.append(jnp.sum(d * d, -1, keepdims=True))
    mean = sum(means) * (1.0 / count)
    square = sum(squares) + step * sum((m - mean) * (m - mean) for m in means)
    return mean, lax.rsqrt(square * (1.0 / width) + norm_eps)


def middle(late, layer, att, wo, x, gain, shift, wk, wv, y, kv, total):
    def run():
        width = x.shape[1]
        heads = wk.shape[1]
        mean, scale = out_project(att, wo, x, total)
        step = 512
        keys = values = None
        for c in range(width // step):
            cut = slice(c * step, (c + 1) * step)
            d = (total[:, cut] - mean) * scale * gain[layer : layer + 1, cut] + shift[layer : layer + 1, cut]
            d = d.astype(bf16)
            y[:, cut] = d
            k = matmul(d, wk[cut, :])
            v = matmul(d, wv[cut, :])
            keys = k if keys is None else keys + k
            values = v if values is None else values + v
        kv[:, :heads] = keys.astype(bf16)
        kv[:, heads:] = values.astype(bf16)

    when_class(late, run)


def last(layer, att, wo, x, gain, shift, out, total, held, sem):
    half = out.shape[1]
    mean, scale = out_project(att, wo, x, total)
    start = lax.axis_index("tp") * half
    parts = sem.shape[0]
    step = half // parts
    copies = []
    for c in range(parts):
        cut = pl.ds(pl.multiple_of(start + c * step, 128), step)
        g = gain[layer : layer + 1, cut]
        s = shift[layer : layer + 1, cut]
        here = slice(c * step, (c + 1) * step)
        held[:, here] = ((total[:, cut] - mean) * scale * g + s).astype(bf16)
        copy = pltpu.make_async_copy(held.at[:, here], out.at[:, here], sem.at[c])
        copy.start()
        copies.append(copy)
    for copy in copies:
        copy.wait()


def body(tokens, wq, wk, wv, wo, table, gain, shift):
    rows, width = tokens.shape
    cols = wq.shape[2]
    heads = table.shape[1]
    count = lax.axis_size("sp")
    flows = [(s, s + 1) for s in range(count - 1)]
    flat_table = table.reshape(LAYERS * heads, table.shape[2])
    tokens, wq, wk, wv, wo = (
        pltpu.with_memory_space_constraint(a, pltpu.HBM) for a in (tokens, wq, wk, wv, wo)
    )
    kv_shape = ((rows, 2 * cols), bf16)
    x_shape = ((rows, width), bf16)
    q_shape = ((rows, cols), bf16)
    in_shape = (wk.shape[1:], bf16)
    out_shape = (wo.shape[1:], bf16)
    ext = pltpu.VMEM((2 * rows, 2 * cols), bf16)
    total = pltpu.VMEM((rows, width), f32)
    dma = pltpu.SemaphoreType.DMA
    weight = pltpu.VMEM((width, cols), bf16)

    def early_kv(late):
        return kernel_call(
            functools.partial(first_kv, late), [kv_shape, x_shape], [ANY] * 3, (tokens, wk, wv),
            [weight, weight, dma((3, 4))], flops=10**8,
        )

    def send(value, pairs):
        return lax.ppermute(value, "sp", pairs)

    def exchange(att):
        return lax.all_gather(att, "tp", axis=1, tiled=True)

    def flow(late_source):
        return [f for f in flows if late_position(f[0]) == late_source]

    def mid(late, args):
        return kernel_call(
            functools.partial(middle, late, 0), [x_shape, kv_shape], [VM] * 7, args,
            [total], flops=10**8,
        )

    own_late, x_late = early_kv(True)
    prev_late = send(own_late, flow(True))
    own_main, x_main = early_kv(False)
    prev_main = send(own_main, flow(False))
    q, bias, x, out_w, key_w, value_w = kernel_call(
        functools.partial(first_query, 0),
        [q_shape, ((LAYERS * heads * SEG, SPAN), f32), x_shape, out_shape, in_shape, in_shape],
        [VM] * 2 + [ANY] * 4 + [VM], (x_main, x_late, wq, wo, wk, wv, flat_table), [weight, dma((4,))],
    )
    att = kernel_call(
        functools.partial(main_attention, 0), [q_shape], [VM] * 4,
        (q, own_main, prev_late, bias), [ext],
    )[0]
    full = exchange(att)
    x_main, next_main = mid(False, (full, out_w, x, gain, shift, key_w, value_w))
    from_main = send(next_main, flow(False))
    att = kernel_call(
        functools.partial(late_attention, 0), [q_shape], [VM] * 5,
        (q, own_late, prev_main, prev_late, bias), [ext],
    )[0]
    full = exchange(att)
    x_late, next_late = mid(True, (full, out_w, x, gain, shift, key_w, value_w))
    from_late = send(next_late, flow(True))
    q, x, out_w = kernel_call(
        functools.partial(later_query, 1), [q_shape, x_shape, out_shape],
        [VM] * 2 + [ANY] * 2, (x_main, x_late, wq, wo), [weight, dma((2,))],
    )
    att = kernel_call(
        functools.partial(final_attention, 1), [q_shape], [VM] * 6,
        (q, next_main, next_late, from_main, from_late, bias), [ext],
    )[0]
    full = exchange(att)
    return kernel_call(
        functools.partial(last, 1), [((rows, width // 2), bf16)],
        [VM] * 5, (full, out_w, x, gain, shift),
        [total, pltpu.VMEM((rows, width // 2), bf16), dma((4,))], out_specs=[ANY],
    )[0]


def solution(mesh):
    return jax.shard_map(
        body,
        mesh=mesh,
        in_specs=(
            P("sp", None),
            P(None, None, "tp"),
            P(None, None, "tp"),
            P(None, None, "tp"),
            P(),
            P(None, "tp", None),
            P(),
            P(),
        ),
        out_specs=P("sp", "tp"),
        check_vma=False,
    )
```

```python
import functools

import jax
import jax.numpy as jnp
from jax import lax
from jax.experimental import pallas as pl
from jax.experimental.pallas import tpu as pltpu
from jax.sharding import PartitionSpec as P

SEG = 64
LEFT = 4
CLIP = 128
LAYERS = 2
REACH = LEFT * SEG
SPAN = 384
PART = 256

inverse_residual_scale = 2.0**-0.5
norm_eps = 1e-05
masked_score = -1e30

VM = pl.BlockSpec(memory_space=pltpu.VMEM)
ANY = pl.BlockSpec(memory_space=pltpu.HBM)
bf16 = jnp.bfloat16
f32 = jnp.float32


def kernel_call(body, outs, specs, args, scratch=(), limit=10 << 20, flops=10**9, out_specs=None):
    return pl.pallas_call(
        body,
        out_shape=[jax.ShapeDtypeStruct(s, d) for s, d in outs],
        in_specs=specs,
        out_specs=out_specs or [VM] * len(outs),
        scratch_shapes=scratch,
        compiler_params=pltpu.CompilerParams(vmem_limit_bytes=limit),
        cost_estimate=pl.CostEstimate(flops=flops, transcendentals=0, bytes_accessed=1 << 20),
    )(*args)


def is_late(position):
    even = jnp.logical_and(lax.rem(position, 2) == 0, position > 0)
    return jnp.logical_or(even, position == 1)


def late_position(position):
    return position == 1 or (position % 2 == 0 and position > 0)


def matmul(a, b):
    return jnp.dot(a, b, preferred_element_type=f32)


def when_class(late, run):
    flag = is_late(lax.axis_index("sp"))
    pl.when(flag if late else jnp.logical_not(flag))(run)


def fetch(pairs, sem):
    copies = [pltpu.make_async_copy(a, b, sem.at[i]) for i, (a, b) in enumerate(pairs)]
    for copy in copies:
        copy.start()
    return copies


def first_kv(late, tok, wk, wv, kv, tokv, wks, wvs, sem):
    def run():
        _, width = tok.shape
        heads = wk.shape[2]
        parts = sem.shape[1]
        step = width // parts
        copies = []
        for c in range(parts):
            cut = pl.ds(c * step, step)
            trio = (
                pltpu.make_async_copy(tok.at[:, cut], tokv.at[:, cut], sem.at[0, c]),
                pltpu.make_async_copy(wk.at[0, cut, :], wks.at[cut, :], sem.at[1, c]),
                pltpu.make_async_copy(wv.at[0, cut, :], wvs.at[cut, :], sem.at[2, c]),
            )
            for copy in trio:
                copy.start()
            copies.append(trio)
        keys = values = None
        for c in range(parts):
            for copy in copies[c]:
                copy.wait()
            cut = pl.ds(c * step, step)
            x = tokv[:, cut]
            k = matmul(x, wks[cut, :])
            v = matmul(x, wvs[cut, :])
            keys = k if keys is None else keys + k
            values = v if values is None else values + v
        kv[:, :heads] = keys.astype(bf16)
        kv[:, heads:] = values.astype(bf16)

    when_class(late, run)


def fill_bias(table, bias):
    rows, cols = table.shape
    t = table[...]
    head = t[:, : cols - 1]
    offset = lax.broadcasted_iota(jnp.int32, (cols - 1, SPAN), 1)
    index = lax.broadcasted_iota(jnp.int32, (cols - 1, SPAN), 0)
    onehot = (jnp.clip(REACH + SEG - 1 - offset, -CLIP, CLIP) + CLIP == index).astype(f32).astype(bf16)
    high = head.astype(bf16)
    rest = head - high.astype(f32)
    mid = rest.astype(bf16)
    low = (rest - mid.astype(f32)).astype(bf16)
    by_offset = matmul(high, onehot) + matmul(mid, onehot) + matmul(low, onehot)
    far = lax.broadcasted_iota(jnp.int32, (rows, SPAN), 1) <= REACH + SEG - 1 - CLIP
    by_offset = jnp.where(far, t[:, cols - 1 :], by_offset)
    first = lax.axis_index("sp") == 0
    for r in range(rows):
        line = jnp.broadcast_to(by_offset[r : r + 1, :], (SEG, SPAN))
        for place, begin in enumerate((0, 2 * SEG, SEG)):
            skew = pltpu.roll(line, SPAN - (SEG - 1) - begin, 1, stride=1, stride_axis=0)[:, :PART]
            if place == 0:
                skew = jnp.where(first, masked_score, skew)
            bias[r * SEG : (r + 1) * SEG, place * PART : (place + 1) * PART] = skew


def scaled_query(x, w):
    return (matmul(x, w).astype(bf16).astype(f32) * 0.125).astype(bf16)


def choose(main, late, out):
    def from_main():
        out[...] = main[...]

    def from_late():
        out[...] = late[...]

    when_class(False, from_main)
    when_class(True, from_late)


def stacked(q, i, heads):
    qs = q[i * SEG : (i + 1) * SEG, :]
    lane = lax.broadcasted_iota(jnp.int32, qs.shape, 1) // (qs.shape[1] // heads)
    return jnp.concatenate([jnp.where(lane == h, qs, jnp.zeros_like(qs)) for h in range(heads)], axis=0)


def by_head(value, width, heads):
    lane = lax.broadcasted_iota(jnp.int32, (SEG, width), 1) // (width // heads)
    picked = value[(heads - 1) * SEG :, :]
    for h in reversed(range(heads - 1)):
        picked = jnp.where(lane == h, value[h * SEG : (h + 1) * SEG, :], picked)
    return picked


def widened(value, width):
    return jnp.concatenate([value] * -(-width // 128), axis=1)[:, :width]


def scores(stack, keys, bias):
    return lax.dot_general(stack, keys, (((1,), (1,)), ((), ())), preferred_element_type=f32) + bias


def staged(steps):
    for _ in range(3):
        for step in steps:
            next(step)


def attend_own(layer, heads, q, own, bias, part, stat):
    rows, width = q.shape
    here = slice(layer * heads * SEG, (layer + 1) * heads * SEG)

    def segment(i):
        known = (i + 1) * SEG
        table = 2 * PART if i % 2 else PART
        begin = table + (2 * SEG if i < 2 else 0)
        score = scores(stacked(q, i, heads), own[:known, :width], bias[here, begin : begin + known])
        yield
        peak = jnp.max(score, -1, keepdims=True)
        expo = jnp.exp(score - peak)
        lines = slice(i * heads * SEG, (i + 1) * heads * SEG)
        stat[lines, :128] = jnp.broadcast_to(peak, (heads * SEG, 128))
        stat[lines, 128:] = jnp.broadcast_to(jnp.sum(expo, -1, keepdims=True), (heads * SEG, 128))
        expo = expo.astype(bf16)
        yield
        part[i * SEG : (i + 1) * SEG, :] = by_head(matmul(expo, own[:known, width:]), width, heads)
        yield

    staged([segment(i) for i in range(rows // SEG)])


def attend_earlier(layer, heads, q, prev, bias, part, stat, out):
    rows, width = q.shape
    here = slice(layer * heads * SEG, (layer + 1) * heads * SEG)

    def segment(i):
        begin = i * SEG
        score = scores(stacked(q, i, heads), prev[begin:, :width], bias[here, : rows - begin])
        yield
        lines = slice(i * heads * SEG, (i + 1) * heads * SEG)
        own_peak = stat[lines, :128]
        peak = jnp.maximum(own_peak, jnp.max(score, -1, keepdims=True))
        expo = jnp.exp(score - widened(peak, rows - begin))
        kept = jnp.exp(own_peak - peak)
        scale = inverse_residual_scale / (kept * stat[lines, 128:] + jnp.sum(expo, -1, keepdims=True))
        expo = expo.astype(bf16)
        yield
        mixed = by_head(matmul(expo, prev[begin:, width:]) * widened(scale, width), width, heads)
        own_mixed = part[i * SEG : (i + 1) * SEG, :] * by_head(widened(kept * scale, width), width, heads)
        out[i * SEG : (i + 1) * SEG, :] = (mixed + own_mixed).astype(bf16)
        yield

    staged([segment(i) for i in range(rows // SEG)])


def first_query(layer, heads, x_main, x_late, own_main, own_late, wq, wo, wk, wv, table, *rest):
    q, bias, x, part, stat, wo0, wk1, wv1, wqs, own, sem = rest
    copies = fetch(
        ((wq.at[layer], wqs), (wo.at[layer], wo0), (wk.at[layer + 1], wk1), (wv.at[layer + 1], wv1)), sem
    )
    choose(x_main, x_late, x)
    choose(own_main, own_late, own)
    fill_bias(table, bias)
    copies[0].wait()
    q[...] = scaled_query(x[...], wqs[...])
    attend_own(layer, heads, q, own, bias, part, stat)
    for copy in copies[1:]:
        copy.wait()


def later_query(layer, heads, x_main, x_late, own_main, own_late, wq, wo, bias, q, x, part, stat, wo1, wqs, own, sem):
    copies = fetch(((wq.at[layer], wqs), (wo.at[layer], wo1)), sem)
    choose(x_main, x_late, x)
    choose(own_main, own_late, own)
    copies[0].wait()
    q[...] = scaled_query(x[...], wqs[...])
    attend_own(layer, heads, q, own, bias, part, stat)
    copies[1].wait()


def choose_source(main, late, out):
    late_source = is_late(lax.axis_index("sp") - 1)

    @pl.when(late_source)
    def _():
        out[...] = late[...]

    @pl.when(jnp.logical_not(late_source))
    def _():
        out[...] = main[...]


def main_attention(layer, heads, q, prev, bias, part, stat, out):
    when_class(False, lambda: attend_earlier(layer, heads, q, prev, bias, part, stat, out))


def late_attention(layer, heads, q, prev_main, prev_late, bias, part, stat, out, prev):
    def run():
        choose_source(prev_main, prev_late, prev)
        attend_earlier(layer, heads, q, prev, bias, part, stat, out)

    when_class(True, run)


def final_attention(layer, heads, q, prev_main, prev_late, bias, part, stat, out, prev):
    choose_source(prev_main, prev_late, prev)
    attend_earlier(layer, heads, q, prev, bias, part, stat, out)


def out_project(att, wo, x, total):
    width = x.shape[1]
    step = 512
    count = width // step
    a = att[...]
    means, squares = [], []
    for c in range(count):
        cut = slice(c * step, (c + 1) * step)
        t = x[:, cut].astype(f32) + matmul(a, wo[:, cut])
        total[:, cut] = t
        m = jnp.sum(t, -1, keepdims=True) * (1.0 / step)
        d = t - m
        means.append(m)
        squares.append(jnp.sum(d * d, -1, keepdims=True))
    mean = sum(means) * (1.0 / count)
    square = sum(squares) + step * sum((m - mean) * (m - mean) for m in means)
    return mean, lax.rsqrt(square * (1.0 / width) + norm_eps / 2)


def middle(late, layer, att, wo, x, gain, shift, wk, wv, y, kv, total):
    def run():
        width = x.shape[1]
        heads = wk.shape[1]
        mean, scale = out_project(att, wo, x, total)
        step = 512
        keys = values = None
        for c in range(width // step):
            cut = slice(c * step, (c + 1) * step)
            d = (total[:, cut] - mean) * scale * gain[layer : layer + 1, cut] + shift[layer : layer + 1, cut]
            d = d.astype(bf16)
            y[:, cut] = d
            k = matmul(d, wk[cut, :])
            v = matmul(d, wv[cut, :])
            keys = k if keys is None else keys + k
            values = v if values is None else values + v
        kv[:, :heads] = keys.astype(bf16)
        kv[:, heads:] = values.astype(bf16)

    when_class(late, run)


def last(layer, att, wo, x, gain, shift, out, total, held, sem):
    half = out.shape[1]
    mean, scale = out_project(att, wo, x, total)
    start = lax.axis_index("tp") * half
    parts = sem.shape[0]
    step = half // parts
    copies = []
    for c in range(parts):
        cut = pl.ds(pl.multiple_of(start + c * step, 128), step)
        g = gain[layer : layer + 1, cut]
        s = shift[layer : layer + 1, cut]
        here = slice(c * step, (c + 1) * step)
        held[:, here] = ((total[:, cut] - mean) * scale * g + s).astype(bf16)
        copy = pltpu.make_async_copy(held.at[:, here], out.at[:, here], sem.at[c])
        copy.start()
        copies.append(copy)
    for copy in copies:
        copy.wait()


def body(tokens, wq, wk, wv, wo, table, gain, shift):
    rows, width = tokens.shape
    cols = wq.shape[2]
    heads = table.shape[1]
    count = lax.axis_size("sp")
    flows = [(s, s + 1) for s in range(count - 1)]
    flat_table = table.reshape(LAYERS * heads, table.shape[2])
    tokens, wq, wk, wv, wo = (
        pltpu.with_memory_space_constraint(a, pltpu.HBM) for a in (tokens, wq, wk, wv, wo)
    )
    kv_shape = ((rows, 2 * cols), bf16)
    x_shape = ((rows, width), bf16)
    q_shape = ((rows, cols), bf16)
    in_shape = (wk.shape[1:], bf16)
    out_shape = (wo.shape[1:], bf16)
    halo = pltpu.VMEM((rows, 2 * cols), bf16)
    bias_shape = ((LAYERS * heads * SEG, 3 * PART), f32)
    part_shape = ((rows, cols), f32)
    stat_shape = ((rows * heads, 256), f32)
    total = pltpu.VMEM((rows, width), f32)
    dma = pltpu.SemaphoreType.DMA
    weight = pltpu.VMEM((width, cols), bf16)

    def early_kv(late):
        return kernel_call(
            functools.partial(first_kv, late), [kv_shape, x_shape], [ANY] * 3, (tokens, wk, wv),
            [weight, weight, dma((3, 4))], flops=10**8,
        )

    def send(value, pairs):
        return lax.ppermute(value, "sp", pairs)

    def exchange(att):
        return lax.all_gather(att, "tp", axis=1, tiled=True)

    def flow(late_source):
        return [f for f in flows if late_position(f[0]) == late_source]

    def mid(late, args):
        return kernel_call(
            functools.partial(middle, late, 0), [x_shape, kv_shape], [VM] * 7, args,
            [total], flops=10**8,
        )

    own_late, x_late = early_kv(True)
    prev_late = send(own_late, flow(True))
    own_main, x_main = early_kv(False)
    prev_main = send(own_main, flow(False))
    q, bias, x, part, stat, out_w, key_w, value_w = kernel_call(
        functools.partial(first_query, 0, heads),
        [q_shape, bias_shape, x_shape, part_shape, stat_shape, out_shape, in_shape, in_shape],
        [VM] * 4 + [ANY] * 4 + [VM], (x_main, x_late, own_main, own_late, wq, wo, wk, wv, flat_table),
        [weight, halo, dma((4,))],
    )
    att = kernel_call(
        functools.partial(main_attention, 0, heads), [q_shape], [VM] * 5,
        (q, prev_late, bias, part, stat),
    )[0]
    full = exchange(att)
    x_main, next_main = mid(False, (full, out_w, x, gain, shift, key_w, value_w))
    from_main = send(next_main, flow(False))
    att = kernel_call(
        functools.partial(late_attention, 0, heads), [q_shape], [VM] * 6,
        (q, prev_main, prev_late, bias, part, stat), [halo],
    )[0]
    full = exchange(att)
    x_late, next_late = mid(True, (full, out_w, x, gain, shift, key_w, value_w))
    from_late = send(next_late, flow(True))
    q, x, part, stat, out_w = kernel_call(
        functools.partial(later_query, 1, heads),
        [q_shape, x_shape, part_shape, stat_shape, out_shape], [VM] * 4 + [ANY] * 2 + [VM],
        (x_main, x_late, next_main, next_late, wq, wo, bias), [weight, halo, dma((2,))],
    )
    att = kernel_call(
        functools.partial(final_attention, 1, heads), [q_shape], [VM] * 6,
        (q, from_main, from_late, bias, part, stat), [halo],
    )[0]
    full = exchange(att)
    return kernel_call(
        functools.partial(last, 1), [((rows, width // 2), bf16)],
        [VM] * 5, (full, out_w, x, gain, shift),
        [total, pltpu.VMEM((rows, width // 2), bf16), dma((4,))], out_specs=[ANY],
    )[0]


def solution(mesh):
    return jax.shard_map(
        body,
        mesh=mesh,
        in_specs=(
            P("sp", None),
            P(None, None, "tp"),
            P(None, None, "tp"),
            P(None, None, "tp"),
            P(),
            P(None, "tp", None),
            P(),
            P(),
        ),
        out_specs=P("sp", "tp"),
        check_vma=False,
    )
```
